128 devices in a mesh: ep: 32 (over z, y, core), tp: 4 (over x).
Axes of the slice: x: 4, y: 4, z: 4, core: 2. Of those that a mesh axis runs over, the one named last changes fastest.
Arguments:
- value_in: bfloat16 [16384, 2048], P('ep', 'tp'), may hold values from -400 to 400
- gate_in: bfloat16 [16384, 2048], P('ep', 'tp'), may hold values from -8 to 8
- conv_taps: float32 [31, 2048], P(None, 'tp'), may hold values from -1 to 1
- conv_bias: float32 [2048], P('tp'), may hold values from -3 to 3
- ln_gain: float32 [2048], P('tp'), may hold values from 0.1 to 1.9
- ln_bias: float32 [2048], P('tp'), may hold values from -3 to 3
- out_proj: bfloat16 [2048, 4096], P('tp'), may hold values from -0.125 to 0.125
- tokens_b: bfloat16 [16384, 4096], P('ep'), may hold values from -6 to 6
- norm_gain: float32 [4096], replicated, may hold values from 0.1 to 1.9
- routes: int32 [16384, 2], P(('ep', 'tp')), may hold values from 0 to 31, all different within a row; in each aligned block of 128 rows (0 to 127, 128 to 255, ...) at most 12 rows name the same one
- route_weights: float32 [16384, 2], P(('ep', 'tp')), may hold values from 0.2 to 1.5
- expert_gate: bfloat16 [32, 4096, 1024], P('ep', None, 'tp'), may hold values from -0.09375 to 0.09375
- expert_up: bfloat16 [32, 4096, 1024], P('ep', None, 'tp'), may hold values from -0.09375 to 0.09375
- expert_down: bfloat16 [32, 1024, 4096], P('ep', 'tp'), may hold values from -0.1875 to 0.1875
- shared_gate: bfloat16 [4096, 1024], P(None, 'tp'), may hold values from -0.09375 to 0.09375
- shared_up: bfloat16 [4096, 1024], P(None, 'tp'), may hold values from -0.09375 to 0.09375
- shared_down: bfloat16 [1024, 4096], P('tp'), may hold values from -0.1875 to 0.1875
Outputs:
- mixer_out: bfloat16 [16384, 4096], P(('ep', 'tp'))
- experts_out: bfloat16 [16384, 4096], P(('ep', 'tp'))
The draws below stay inside these ranges and needn't reach their ends.
Inputs may be any that keep to these rules, and one draw needn't show every extreme that they name: `routes`: each row names 2 different experts. In each aligned block of 128 rows (the rows of one device) no expert is named by more than 12 rows, and in some blocks an expert is named by exactly 12 rows.
All inputs are finite; a program needn't handle non-finite values.
Results may differ from the reference program's by a relative error of at most 0.012.
Values may be sent and summed in bfloat16 or wider, within the bound.
No kernel may reach another device: no remote copies, remote signals or barrier semaphores. Data moves between devices by JAX's collectives and lax.ppermute only.
A program may use at most 128 MiB of HBM per device.

```python
import math
from functools import partial
import jax
import jax.numpy as jnp
import numpy as np
from jax import lax

D = 4096
CHANNELS = 2048
EXPERT_WIDTH = 1024
TAPS = 31
TOP_K = 2
ROWS_DEV = 128
EXPERTS = 32
CAP = 12
SEQ_LEN = 16384
TOKENS_B = 16384
N_TP = 4


def draw_value_in(key, part):
    keys = jax.random.split(jax.random.fold_in(key, 11), 2)
    base = jnp.clip(jax.random.normal(keys[0], (SEQ_LEN, CHANNELS), jnp.float32), -5.0, 5.0)
    column = jnp.arange(CHANNELS, dtype=jnp.float32) / CHANNELS
    rough = jax.random.uniform(keys[1], (CHANNELS,), jnp.float32, 0.5, 1.5)
    scales = 0.3 * 10.0 ** column * rough
    values = base * scales[None, :]
    return values.astype(jnp.bfloat16)


def levels(key, dims, shards, least, largest):
    gain, own = 1.0, jax.random.fold_in(key, 6)
    for position, shards_of in shards:
        draws = jnp.exp(jax.random.uniform(jax.random.fold_in(own, position), (shards_of,), jnp.float32, least / len(shards), largest / len(shards)))
        gain = gain * jnp.repeat(draws, dims[position] // shards_of).reshape([-1 if axis == position else 1 for axis in range(len(dims))])
    return gain


def deal_out(rng, own, number, rows, amount, top, limit, lean):
    order = jax.random.permutation(rng, amount)
    heavy_load, ordinary = load_shares(amount, rows * top, limit, lean, True), load_shares(amount, rows * top, limit, lean, False)
    places = jnp.arange(amount)

    def named(sizes, offset_by):
        used = int((sizes > 0).sum())
        fixed = max(1, used // 4)
        shifted = fixed + (places - fixed + offset_by * (used - fixed)) % max(1, amount - fixed)
        return jnp.zeros((amount,), jnp.int32).at[order[jnp.where(places < fixed, places, shifted)]].set(jnp.asarray(sizes, jnp.int32))

    sizes = jnp.where(number % 4 == 0, named(heavy_load, number // 4), named(ordinary, number - number // 4 - 1))
    mixed = jax.random.permutation(jax.random.fold_in(own, 3), amount)
    giver, sink = mixed[0:amount // 2 * 2:2], mixed[1:amount // 2 * 2:2]
    slack = jnp.minimum(sizes[giver] - 1, limit - sizes[sink]) // 2
    slack = jnp.where((giver == order[0]) | (sink == order[0]) | (sizes[sink] == 0), 0, jnp.maximum(slack, 0))
    shifted = jax.random.randint(jax.random.fold_in(own, 4), (amount // 2,), 0, 1 << 20) % (slack + 1)
    sizes = sizes.at[giver].add(-shifted).at[sink].add(shifted)
    labels = jnp.searchsorted(jnp.cumsum(sizes), jnp.arange(rows * top), side="right").astype(jnp.int32)
    table = labels.reshape(top, rows).T
    table = table[jax.random.permutation(jax.random.fold_in(own, 1), rows)]
    offset_by = jax.random.randint(jax.random.fold_in(own, 2), (rows, 1), 0, top)
    return jnp.take_along_axis(table, (jnp.arange(top)[None, :] + offset_by) % top, axis=1)


def load_shares(number_of, total, most, lean, full):
    portions = [(1 << 20) // math.isqrt(rank ** lean) + 1 for rank in range(1, number_of + 1)]
    largest = most if full else min(most, max(-(-total // number_of), total * portions[0] // sum(portions)))
    least = 1 if total - largest >= number_of - 1 else 0
    holding, rest = [largest] + [least] * (number_of - 1), total - largest - least * (number_of - 1)
    while rest > 0:
        free = [i for i in range(1, number_of) if holding[i] < largest] or [i for i in range(1, number_of) if holding[i] < most]
        whole, left = sum([portions[i] for i in free]), rest
        for i in free:
            addition = min(most - holding[i], max(1, left * portions[i] // whole), rest)
            holding[i] = holding[i] + addition
            rest = rest - addition
    return np.array(holding)


def normal_values(key, dims, deviation, bound, pieces=(), kind=jnp.bfloat16):
    values = jax.random.normal(key, dims, jnp.float32) * deviation
    if len(pieces) > 0:
        values = levels(key, dims, pieces, -0.22, 0.18) * values
    return jnp.clip(values, min=-bound, max=bound).astype(kind)


def setup_inputs(seed: int = 0) -> dict:
    key_of = jax.random.split(jax.random.key(seed), 18)
    value_in = draw_value_in(jax.random.fold_in(key_of[17], 71), 0)
    gate_in = normal_values(key_of[1], (SEQ_LEN, CHANNELS), 1.5, 8.0, ((0, 32), (1, 4)))
    conv_taps = normal_values(key_of[2], (TAPS, CHANNELS), TAPS ** -0.5, 1.0, ((1, 4),), jnp.float32)
    conv_bias = normal_values(key_of[3], (CHANNELS,), 0.5, 3.0, ((0, 4),), jnp.float32)
    ln_gain = jnp.clip(1.0 + 0.18 * jax.random.normal(key_of[4], (CHANNELS,), jnp.float32), 0.1, 1.9)
    ln_bias = normal_values(key_of[5], (CHANNELS,), 0.5, 3.0, ((0, 4),), jnp.float32)
    out_proj = normal_values(key_of[6], (CHANNELS, D), CHANNELS ** -0.5, 0.125, ((0, 4),))
    tokens_b = normal_values(key_of[7], (TOKENS_B, D), 1.0, 6.0, ((0, 32),))
    norm_gain = jnp.clip(1.0 + 0.18 * jax.random.normal(key_of[8], (D,), jnp.float32), 0.1, 1.9)
    routes_keys = jax.random.split(jax.random.fold_in(key_of[9], 1), TOKENS_B // ROWS_DEV)
    routes_turns = jax.random.permutation(jax.random.fold_in(key_of[9], 3), TOKENS_B // ROWS_DEV)
    routes = jax.vmap(lambda own, number: deal_out(jax.random.fold_in(key_of[9], 2), own, number, ROWS_DEV, EXPERTS, TOP_K, CAP, 1))(routes_keys, routes_turns).reshape((TOKENS_B, TOP_K))
    route_weights = jnp.clip(0.2 + 1.3 * jax.random.uniform(key_of[10], (TOKENS_B, TOP_K), jnp.float32) ** levels(key_of[10], (TOKENS_B, TOP_K), ((0, 128),), -0.2, 0.2), 0.2, 1.5)
    expert_gate = normal_values(key_of[11], (EXPERTS, D, EXPERT_WIDTH), D ** -0.5, 0.09375, ((0, 32), (2, 4)))
    expert_up = normal_values(key_of[12], (EXPERTS, D, EXPERT_WIDTH), D ** -0.5, 0.09375, ((0, 32), (2, 4)))
    expert_down = normal_values(key_of[13], (EXPERTS, EXPERT_WIDTH, D), EXPERT_WIDTH ** -0.5, 0.1875, ((0, 32), (1, 4)))
    shared_gate = normal_values(key_of[14], (D, EXPERT_WIDTH), D ** -0.5, 0.09375, ((1, 4),))
    shared_up = normal_values(key_of[15], (D, EXPERT_WIDTH), D ** -0.5, 0.09375, ((1, 4),))
    shared_down = normal_values(key_of[16], (EXPERT_WIDTH, D), EXPERT_WIDTH ** -0.5, 0.1875, ((0, 4),))
    return dict(value_in=value_in, gate_in=gate_in, conv_taps=conv_taps, conv_bias=conv_bias, ln_gain=ln_gain, ln_bias=ln_bias, out_proj=out_proj, tokens_b=tokens_b, norm_gain=norm_gain, routes=routes, route_weights=route_weights, expert_gate=expert_gate, expert_up=expert_up, expert_down=expert_down, shared_gate=shared_gate, shared_up=shared_up, shared_down=shared_down)


EPSILON = 1e-06

def round_trip(values):
    return lax.optimization_barrier(values.astype(jnp.bfloat16)).astype(jnp.float32)

def blocked_product(hidden, weight):
    block_rows = hidden.shape[1] // N_TP
    summed = jnp.zeros((hidden.shape[0], weight.shape[1]), jnp.float32)
    for block in range(N_TP):
        partial_sum = jnp.dot(hidden[:, block * block_rows:(block + 1) * block_rows], weight[block * block_rows:(block + 1) * block_rows], preferred_element_type=jnp.float32)
        summed = summed + round_trip(partial_sum)
    return summed.astype(jnp.bfloat16)

def gated_ffn(rows_in, weight_gate, weight_up, weight_down):
    hidden = (jax.nn.silu(jnp.dot(rows_in, weight_gate, preferred_element_type=jnp.float32)) * jnp.dot(rows_in, weight_up, preferred_element_type=jnp.float32)).astype(jnp.bfloat16)
    return blocked_product(hidden, weight_down)

def slot_table(route_ids, expert_count):
    chosen = route_ids.reshape(-1)
    onehot = (chosen[:, None] == jnp.arange(expert_count, dtype=jnp.int32)[None, :]).astype(jnp.int32)
    earlier = jnp.cumsum(onehot, axis=0) - onehot
    return (chosen, lax.optimization_barrier(jnp.sum(earlier * onehot, axis=1)).astype(jnp.int32))

def reference(value_in, gate_in, conv_taps, conv_bias, ln_gain, ln_bias, out_proj, tokens_b, norm_gain, routes, route_weights, expert_gate, expert_up, expert_down, shared_gate, shared_up, shared_down):
    gated = round_trip(value_in.astype(jnp.float32) * jax.nn.sigmoid(gate_in.astype(jnp.float32)))
    padded = jnp.concatenate([jnp.zeros((TAPS - 1, CHANNELS), jnp.float32), gated], axis=0)
    filtered = jnp.zeros((SEQ_LEN, CHANNELS), jnp.float32) + conv_bias[None, :]
    for tap_index in range(TAPS):
        filtered = filtered + conv_taps[tap_index][None, :] * padded[tap_index:tap_index + SEQ_LEN]
    average = lax.optimization_barrier(jnp.sum(filtered, axis=1)) / CHANNELS
    variance = lax.optimization_barrier(jnp.sum(filtered * filtered, axis=1)) / CHANNELS - average * average
    normed_a = (filtered - average[:, None]) * lax.rsqrt(variance[:, None] + EPSILON) * ln_gain + ln_bias
    activated = jax.nn.silu(normed_a).astype(jnp.bfloat16)
    mixer_out = blocked_product(activated, out_proj)
    features = tokens_b.astype(jnp.float32)
    normed_b = (features * lax.rsqrt(lax.optimization_barrier(jnp.mean(features * features, axis=1, keepdims=True)) + EPSILON) * norm_gain).astype(jnp.bfloat16)
    block_count = TOKENS_B // ROWS_DEV
    chosen, places = jax.vmap(partial(slot_table, expert_count=EXPERTS))(routes.reshape(block_count, ROWS_DEV * TOP_K))
    row_ids = jnp.arange(block_count, dtype=jnp.int32)[:, None] * ROWS_DEV + jnp.arange(ROWS_DEV * TOP_K, dtype=jnp.int32)[None, :] // TOP_K
    block_grid = jnp.broadcast_to(jnp.arange(block_count, dtype=jnp.int32)[:, None], row_ids.shape)
    slot_rows = jnp.zeros((EXPERTS, block_count, CAP), jnp.int32).at[chosen, block_grid, places].set(row_ids)
    slot_weights = jnp.zeros((EXPERTS, block_count, CAP), jnp.float32).at[chosen, block_grid, places].set(route_weights.reshape(block_count, ROWS_DEV * TOP_K))

    def per_expert(accumulated, inputs):
        weight_gate, weight_up, weight_down, rows_expert, weights_expert = inputs
        picked_ids = rows_expert.reshape(-1)
        outputs = gated_ffn(normed_b[picked_ids], weight_gate, weight_up, weight_down)
        accumulated = accumulated.at[picked_ids].add(outputs.astype(jnp.float32) * weights_expert.reshape(-1)[:, None])
        return (accumulated, None)
    routed, _ = lax.scan(per_expert, jnp.zeros((TOKENS_B, D), jnp.float32), (expert_gate, expert_up, expert_down, slot_rows, slot_weights))
    shared_rows = gated_ffn(normed_b, shared_gate, shared_up, shared_down)
    experts_out = (shared_rows.astype(jnp.float32) + routed).astype(jnp.bfloat16)
    return (mixer_out, experts_out)
```

```python
from functools import partial

import jax
import jax.numpy as jnp
from jax import lax
from jax.experimental import pallas as pl
from jax.experimental.pallas import tpu as pltpu
from jax.sharding import PartitionSpec as P


EPSILON = 1e-06
BF16, F32 = jnp.bfloat16, jnp.float32


def shifted(x, axis, by):
    devices = lax.axis_size(axis)
    pairs = [(i, i + by) for i in range(devices) if 0 <= i + by < devices]
    return lax.ppermute(x, axis, pairs)


def swapped(x, axis, bits):
    return lax.ppermute(x, axis, [(i, i ^ bits) for i in range(lax.axis_size(axis))])


def dot(a, b):
    return jnp.dot(a, b, preferred_element_type=F32)


def dot_rows(a, b):
    return lax.dot_general(a, b, (((1,), (1,)), ((), ())), preferred_element_type=F32)


def gated_product(gate, up):
    return (jax.nn.silu(gate) * up).astype(BF16)


def iota(shape, dim):
    return lax.broadcasted_iota(jnp.int32, shape, dim)


def ones_where(mask):
    return jnp.where(mask, 1.0, 0.0).astype(BF16)


def quotient(x, by):
    return (x * (65536 // by + 1)) >> 16


def places(routes, experts):
    rows = routes.shape[0]
    expert = iota((rows, experts), 1)
    named = (routes[:, 0:1] == expert) | (routes[:, 1:2] == expert)
    earlier = ones_where(iota((rows, rows), 1) < iota((rows, rows), 0))
    return jnp.where(named, dot(earlier, ones_where(named)), -1.0)


def outbox_body(flags, tokens, gain, own, other, out, rows, place, select, *, capacity, chunk):
    step = pl.program_id(0)
    block, width = own.shape[0], gain.shape[1]
    experts = place.shape[1]

    @pl.when(step == 0)
    def _():
        def norm(i, carry):
            at = pl.multiple_of((i % (block // chunk)) * chunk, chunk)
            x = tokens[i // (block // chunk), 0, pl.ds(at, chunk), :].astype(F32)
            scale = lax.rsqrt(jnp.sum(x * x, axis=1, keepdims=True) * (1.0 / width) + EPSILON)
            rows[pl.ds(pl.multiple_of(i * chunk, chunk), chunk), :] = (x * scale * gain[...]).astype(BF16)
            return carry

        lax.fori_loop(0, 2 * block // chunk, norm, 0)
        first = flags[1] == 0
        place[:block, :] = places(jnp.where(first, own[...], other[...]), experts).astype(BF16)
        place[block:, :] = places(jnp.where(first, other[...], own[...]), experts).astype(BF16)
        slots = select.shape[0]
        slot = iota((slots, 1), 0)
        expert = quotient(slot, 2 * capacity)
        within = slot - expert * (2 * capacity)
        second = jnp.where(within >= capacity, 1, 0)
        wanted = (within - second * capacity).astype(F32)
        there = dot_rows(ones_where(expert == iota((slots, experts), 1)), place[...])
        row_block = jnp.where(iota((slots, 2 * block), 1) >= block, 1, 0)
        select[...] = ones_where((there == wanted) & (row_block == second))

    here = out.shape[1]
    at = pl.multiple_of(step * here, here)
    out[...] = dot(select[...], rows[:, pl.ds(at, here)]).astype(BF16)


def outbox_of(flags, tokens, gain, own, other, experts, capacity):
    width = tokens.shape[1]
    block = own.shape[0]
    slots = experts * 2 * capacity
    here = 512
    return pl.pallas_call(
        partial(outbox_body, capacity=capacity, chunk=16),
        grid_spec=pltpu.PrefetchScalarGridSpec(
            num_scalar_prefetch=1,
            grid=(width // here,),
            in_specs=[
                pl.BlockSpec((2, 1, block, width), lambda i, f: (0, f[0], 0, 0)),
                pl.BlockSpec((1, width), lambda i, f: (0, 0)),
                pl.BlockSpec(own.shape, lambda i, f: (0, 0)),
                pl.BlockSpec(other.shape, lambda i, f: (0, 0)),
            ],
            out_specs=pl.BlockSpec((slots, here), lambda i, f: (0, i)),
            scratch_shapes=[
                pltpu.VMEM((2 * block, width), BF16),
                pltpu.VMEM((2 * block, experts), BF16),
                pltpu.VMEM((slots, 2 * block), BF16),
            ],
        ),
        out_shape=jax.ShapeDtypeStruct((slots, width), BF16),
        cost_estimate=pl.CostEstimate(flops=2 * slots * 2 * block * width, bytes_accessed=2 * width * (slots + 2 * block), transcendentals=0),
        name="outbox",
    )(flags, tokens.reshape(2, 2, block, width), gain.reshape(1, width), own, other)


def hidden_body(flags, arrived, gate, up, first, second, kept, sent, sums, hidden, *, capacity, chunk):
    step = pl.program_id(0)
    a = arrived[...]
    weights = (gate, up, first, second)

    @pl.when(step == 0)
    def _():
        for i, w in enumerate(weights):
            sums[i] = dot(a, w[...])

    @pl.when(step != 0)
    def _():
        for i, w in enumerate(weights):
            sums[i] += dot(a, w[...])

    @pl.when(step == pl.num_programs(0) - 1)
    def _():
        units = gate.shape[1]
        half = units // 2

        def activate(i, carry):
            at = pl.ds(pl.multiple_of(i * chunk, chunk), chunk)
            hidden[at, :units] = gated_product(sums[0, at, :], sums[1, at, :])
            hidden[at, units : units + half] = gated_product(sums[2, at, :half], sums[2, at, half:])
            hidden[at, units + half :] = gated_product(sums[3, at, :half], sums[3, at, half:])
            return carry

        lax.fori_loop(0, a.shape[0] // chunk, activate, 0)
        shape = (kept.shape[0], a.shape[0])
        row = iota((shape[0], 1), 0)
        source = row + capacity * quotient(row, capacity)
        lane = iota(shape, 1)
        kept[...] = dot(ones_where(lane == source + capacity * flags[1]), hidden[...]).astype(BF16)
        sent[...] = dot(ones_where(lane == source + capacity * (1 - flags[1])), hidden[...]).astype(BF16)


def hidden_of(flags, arrived, gate, up, first, second, capacity):
    rows, width = arrived.shape
    units = gate.shape[1]
    step = 512
    out = jax.ShapeDtypeStruct((rows // 2, 2 * units), BF16)
    weight = pl.BlockSpec((step, units), lambda k, f: (k, 0))
    whole = pl.BlockSpec(out.shape, lambda k, f: (0, 0))
    return pl.pallas_call(
        partial(hidden_body, capacity=capacity, chunk=64),
        grid_spec=pltpu.PrefetchScalarGridSpec(
            num_scalar_prefetch=1,
            grid=(width // step,),
            in_specs=[pl.BlockSpec((rows, step), lambda k, f: (0, k))] + [weight] * 4,
            out_specs=[whole, whole],
            scratch_shapes=[pltpu.VMEM((4, rows, units), F32), pltpu.VMEM((rows, 2 * units), BF16)],
        ),
        out_shape=[out, out],
        cost_estimate=pl.CostEstimate(flops=8 * rows * width * units, bytes_accessed=2 * width * (rows + 4 * units), transcendentals=0),
        name="hidden",
    )(flags, arrived, gate, up, first, second)


def down_body(flags, kept, got, left, right, out, whole, wide, *, capacity):
    units = whole.shape[1] // 4
    half = units // 2

    @pl.when(pl.program_id(0) == 0)
    def _():
        k, g = kept[...], got[...]
        by_distance = [
            k[:, :units],
            jnp.concatenate([k[:, units : units + half], g[:, units + half :]], axis=1),
            g[:, :units],
            jnp.concatenate([g[:, units : units + half], k[:, units + half :]], axis=1),
        ]
        odd, high = flags[0] == 1, flags[1] == 1
        turned = [jnp.where(odd, by_distance[i ^ 1], by_distance[i]) for i in range(4)]
        for i in range(4):
            whole[:, i * units : (i + 1) * units] = jnp.where(high, turned[i ^ 2], turned[i])

    for side, weight in enumerate((left, right)):
        rows = dot(whole[...], weight[...])
        for expert in range(rows.shape[0] // capacity):
            at = (2 * expert + side) * capacity
            wide[at : at + capacity, :] = rows[expert * capacity : (expert + 1) * capacity, :]
    out[...] = wide[...].astype(BF16)


def down_of(flags, kept, got, down, capacity):
    rows, units = kept.shape[0], down.shape[0]
    width = down.shape[1] // 2
    step = 256
    count = width // step
    whole = pl.BlockSpec(kept.shape, lambda n, f: (0, 0))
    return pl.pallas_call(
        partial(down_body, capacity=capacity),
        grid_spec=pltpu.PrefetchScalarGridSpec(
            num_scalar_prefetch=1,
            grid=(count,),
            in_specs=[
                whole,
                whole,
                pl.BlockSpec((units, step), lambda n, f: (0, n)),
                pl.BlockSpec((units, step), lambda n, f: (0, n + count)),
            ],
            out_specs=pl.BlockSpec((2 * rows, step), lambda n, f: (0, n)),
            scratch_shapes=[pltpu.VMEM((rows, units), BF16), pltpu.VMEM((2 * rows, step), F32)],
        ),
        out_shape=jax.ShapeDtypeStruct((2 * rows, width), BF16),
        cost_estimate=pl.CostEstimate(flops=4 * rows * units * width, bytes_accessed=4 * width * (rows + units), transcendentals=0),
        name="down",
    )(flags, kept, got, down, down)


def product_body(a, b, out):
    out[...] = dot(a[...], b[...]).astype(BF16)


def product_of(a, b):
    rows, width = a.shape[0], b.shape[1]
    block = 128
    return pl.pallas_call(
        product_body,
        grid=(rows // block,),
        in_specs=[pl.BlockSpec((block, a.shape[1]), lambda i: (i, 0)), pl.BlockSpec(b.shape, lambda i: (0, 0))],
        out_specs=pl.BlockSpec((block, width), lambda i: (i, 0)),
        out_shape=jax.ShapeDtypeStruct((rows, width), BF16),
        cost_estimate=pl.CostEstimate(flops=2 * rows * width * b.shape[0], bytes_accessed=2 * width * (rows + b.shape[0]), transcendentals=0),
    )(a, b)


def shared_body(flags, hidden, down, send_1, keep_1, send_3, keep_3):
    me = flags[0] + 2 * flags[1]
    block, width = send_1.shape[0] // 2, send_1.shape[1]
    targets = (
        ((keep_1, 0), (keep_3, 0)),
        ((send_1, 0), (keep_3, 1)),
        ((send_1, 1), (send_3, 1)),
        ((keep_1, 1), (send_3, 0)),
    )
    for away, sides in enumerate(targets):
        at = pl.multiple_of((me ^ away) * block, block)
        for side, (out, place) in enumerate(sides):
            product = dot(hidden[pl.ds(at, block), :], down[:, side * width : (side + 1) * width])
            out[place * block : (place + 1) * block, :] = product.astype(BF16)


def shared_parts_of(flags, hidden, down):
    rows, width = hidden.shape[0], down.shape[1]
    out = jax.ShapeDtypeStruct((rows // 2, width // 2), BF16)
    whole = pl.BlockSpec(out.shape, lambda i, f: (0, 0))
    return pl.pallas_call(
        shared_body,
        grid_spec=pltpu.PrefetchScalarGridSpec(
            num_scalar_prefetch=1,
            grid=(1,),
            in_specs=[pl.BlockSpec(hidden.shape, lambda i, f: (0, 0)), pl.BlockSpec(down.shape, lambda i, f: (0, 0))],
            out_specs=[whole] * 4,
        ),
        out_shape=[out] * 4,
        cost_estimate=pl.CostEstimate(flops=2 * rows * width * down.shape[0], bytes_accessed=2 * width * (rows + down.shape[0]), transcendentals=0),
        name="shared_product",
    )(flags, hidden, down)


def portions_body(routes, weights, mix, *, capacity, experts):
    block, slots = routes.shape[0], mix.shape[2]
    chosen = routes[...]
    expert = iota((block, experts), 1)
    weight = jnp.where(chosen[:, 0:1] == expert, weights[:, 0:1], 0.0) + jnp.where(
        chosen[:, 1:2] == expert, weights[:, 1:2], 0.0
    )
    upper = weight.astype(BF16)
    lower = (weight - upper.astype(F32)).astype(BF16)
    lane = iota((experts, slots), 1)
    unfold = ones_where(quotient(lane, 2 * capacity) == iota((experts, slots), 0))
    lane = iota((1, slots), 1)
    within = lane - quotient(lane, 2 * capacity) * (2 * capacity)
    second = jnp.where(within >= capacity, 1, 0)
    wanted = (within - second * capacity).astype(F32)
    hit = dot(places(chosen, experts).astype(BF16), unfold) == wanted
    for part, values in enumerate((upper, lower)):
        there = dot(values, unfold)
        for side in range(2):
            mix[side, part * block : (part + 1) * block, :] = jnp.where(
                hit & (second == side), there, 0.0
            ).astype(BF16)


def portions_of(routes, weights, experts, capacity):
    block, slots = routes.shape[0], 2 * experts * capacity
    return pl.pallas_call(
        partial(portions_body, capacity=capacity, experts=experts),
        out_shape=jax.ShapeDtypeStruct((2, 2 * block, slots), BF16),
        cost_estimate=pl.CostEstimate(flops=6 * block * slots * experts, bytes_accessed=8 * block * slots, transcendentals=0),
        name="portions",
    )(routes, weights)


def mix_body(portions, returned, shared, out):
    block = out.shape[0]
    both = dot(portions[pl.program_id(1)], returned[...])
    out[...] = (shared[...].astype(F32) + (both[:block] + both[block:])).astype(BF16)


def mixed_of(portions, returned, shared):
    slots, width = returned.shape
    block = shared.shape[0]
    step = 512
    count = width // step
    return pl.pallas_call(
        mix_body,
        grid=(count, 2),
        in_specs=[
            pl.BlockSpec(portions.shape, lambda n, h: (0, 0, 0)),
            pl.BlockSpec((slots, step), lambda n, h: (0, n)),
            pl.BlockSpec((block, step), lambda n, h: (0, h * count + n)),
        ],
        out_specs=pl.BlockSpec((block, step), lambda n, h: (0, h * count + n)),
        out_shape=jax.ShapeDtypeStruct((block, 2 * width), BF16),
        cost_estimate=pl.CostEstimate(flops=8 * block * slots * width, bytes_accessed=2 * width * (slots + 4 * block), transcendentals=0),
        name="mix",
    )(portions, returned, shared)


def gated_of(value_in, gate_in):
    return (value_in.astype(F32) * jax.nn.sigmoid(gate_in.astype(F32))).astype(BF16)


def convolved(before, gated, conv_taps, conv_bias):
    length = gated.shape[0]
    padded = jnp.concatenate([before, gated], axis=0).astype(F32)
    filtered = jnp.zeros(gated.shape, F32) + conv_bias[None, :]
    for tap_index in range(conv_taps.shape[0]):
        filtered = filtered + conv_taps[tap_index][None, :] * padded[tap_index : tap_index + length]
    return filtered


def per_device(
    value_in,
    gate_in,
    conv_taps,
    conv_bias,
    ln_gain,
    ln_bias,
    out_proj,
    tokens_b,
    norm_gain,
    routes,
    route_weights,
    expert_gate,
    expert_up,
    expert_down,
    shared_gate,
    shared_up,
    shared_down,
):
    tp_count = lax.axis_size("tp")
    ep_count = lax.axis_size("ep")
    me = lax.axis_index("tp")
    flags = jnp.stack([me & 1, me >> 1]).astype(jnp.int32)
    rows_own, top_count = routes.shape
    capacity = max(2, 3 * rows_own * top_count // (2 * ep_count))
    width = tokens_b.shape[1]
    gate_local, up_local, down_local = expert_gate[0], expert_up[0], expert_down[0]
    half = gate_local.shape[1] // 2
    down_all = lax.all_gather(down_local, "tp", axis=0, tiled=True)

    other_routes = swapped(routes, "tp", 2)

    rim = value_in.shape[0] - (conv_taps.shape[0] - 1)
    tail = gated_of(value_in[rim:], gate_in[rim:])
    before = shifted(tail, "ep", 1)

    first = jnp.concatenate([gate_local[:, :half], up_local[:, :half]], axis=1)
    second = jnp.concatenate([gate_local[:, half:], up_local[:, half:]], axis=1)
    first_of_1 = swapped(first, "tp", 1)
    second_of_3 = swapped(second, "tp", 3)

    outbox = outbox_of(flags, tokens_b, norm_gain, routes, other_routes, ep_count, capacity)
    arrived = lax.all_to_all(
        outbox.reshape(ep_count, 2 * capacity, width), "ep", split_axis=0, concat_axis=0, tiled=True
    ).reshape(2 * capacity * ep_count, width)
    tokens_b, value_in, gate_in, outbox = lax.optimization_barrier((tokens_b, value_in, gate_in, outbox))

    filtered = convolved(before, gated_of(value_in, gate_in), conv_taps, conv_bias)
    sums = jnp.stack([jnp.sum(filtered, axis=1), jnp.sum(filtered * filtered, axis=1)])
    other_sums = [swapped(sums, "tp", bits) for bits in (1, 2, 3)]

    features = tokens_b.astype(F32)
    normed_b = (
        features
        * lax.rsqrt(jnp.mean(features * features, axis=1, keepdims=True) + EPSILON)
        * norm_gain
    ).astype(BF16)
    hidden_shared = gated_product(dot(normed_b, shared_gate), dot(normed_b, shared_up))
    send_1, keep_1, send_3, keep_3 = shared_parts_of(flags, hidden_shared, shared_down)

    *other_sums, hidden_shared, send_1, send_3 = lax.optimization_barrier(
        (*other_sums, hidden_shared, send_1, send_3)
    )
    total = sums + other_sums[0] + (other_sums[1] + other_sums[2])
    channel_count = filtered.shape[1] * tp_count
    average = total[0] / channel_count
    variance = total[1] / channel_count - average * average
    normed_a = (filtered - average[:, None]) * lax.rsqrt(
        variance[:, None] + EPSILON
    ) * ln_gain + ln_bias
    activated = jax.nn.silu(normed_a).astype(BF16)
    mixer_parts = product_of(activated, out_proj)
    mixer_rows = lax.psum_scatter(mixer_parts, "tp", scatter_dimension=0, tiled=True)

    kept, sent = hidden_of(flags, arrived, gate_local, up_local, first_of_1, second_of_3, capacity)
    got = swapped(sent, "tp", 2)

    left_1 = swapped(send_1, "tp", 1)
    right_1 = swapped(send_3, "tp", 3)

    expert_rows = down_of(flags, kept, got, down_all, capacity)
    returned = lax.all_to_all(
        expert_rows.reshape(ep_count, 2 * capacity, width // 2), "ep", split_axis=0, concat_axis=0, tiled=True
    ).reshape(2 * capacity * ep_count, width // 2)
    left_sum = keep_1.astype(F32) + left_1.astype(F32)
    right_sum = keep_3.astype(F32) + right_1.astype(F32)
    left_on, right_on = left_sum[rows_own:].astype(BF16), right_sum[rows_own:].astype(BF16)
    left_2 = swapped(left_on, "tp", 3)
    right_2 = swapped(right_on, "tp", 1)
    shared_rows = jnp.concatenate(
        [left_sum[:rows_own] + left_2.astype(F32), right_sum[:rows_own] + right_2.astype(F32)], axis=1
    ).astype(BF16)
    portions = portions_of(routes, route_weights, ep_count, capacity)
    experts_out = mixed_of(portions, returned, shared_rows)
    return (mixer_rows, experts_out)


def solution(mesh):
    return jax.shard_map(
        per_device,
        mesh=mesh,
        in_specs=(
            P("ep", "tp"),
            P("ep", "tp"),
            P(None, "tp"),
            P("tp"),
            P("tp"),
            P("tp"),
            P("tp", None),
            P("ep", None),
            P(),
            P(("ep", "tp"), None),
            P(("ep", "tp"), None),
            P("ep", None, "tp"),
            P("ep", None, "tp"),
            P("ep", "tp", None),
            P(None, "tp"),
            P(None, "tp"),
            P("tp", None),
        ),
        out_specs=(P(("ep", "tp"), None), P(("ep", "tp"), None)),
        check_vma=False,
    )
```

```python
from functools import partial

import jax
import jax.numpy as jnp
from jax import lax
from jax.experimental import pallas as pl
from jax.experimental.pallas import tpu as pltpu
from jax.sharding import PartitionSpec as P


EPSILON = 1e-06
BF16, F32 = jnp.bfloat16, jnp.float32


def shifted(x, axis, by):
    devices = lax.axis_size(axis)
    pairs = [(i, i + by) for i in range(devices) if 0 <= i + by < devices]
    return lax.ppermute(x, axis, pairs)


def swapped(x, axis, bits):
    return lax.ppermute(x, axis, [(i, i ^ bits) for i in range(lax.axis_size(axis))])


def dot(a, b):
    return jnp.dot(a, b, preferred_element_type=F32)


def dot_rows(a, b):
    return lax.dot_general(a, b, (((1,), (1,)), ((), ())), preferred_element_type=F32)


def gated_product(gate, up):
    return (jax.nn.silu(gate) * up).astype(BF16)


def iota(shape, dim):
    return lax.broadcasted_iota(jnp.int32, shape, dim)


def ones_where(mask):
    return jnp.where(mask, 1.0, 0.0).astype(BF16)


def quotient(x, by):
    return (x * (65536 // by + 1)) >> 16


def places(routes, experts):
    rows = routes.shape[0]
    expert = iota((rows, experts), 1)
    named = (routes[:, 0:1] == expert) | (routes[:, 1:2] == expert)
    earlier = ones_where(iota((rows, rows), 1) < iota((rows, rows), 0))
    return jnp.where(named, dot(earlier, ones_where(named)), -1.0)


def outbox_body(flags, tokens, gain, own, other, out, rows, place, select, *, capacity, chunk):
    step = pl.program_id(0)
    block, width = own.shape[0], gain.shape[1]
    experts = place.shape[1]

    @pl.when(step == 0)
    def _():
        def norm(i, carry):
            at = pl.multiple_of((i % (block // chunk)) * chunk, chunk)
            x = tokens[i // (block // chunk), 0, pl.ds(at, chunk), :].astype(F32)
            scale = lax.rsqrt(jnp.sum(x * x, axis=1, keepdims=True) * (1.0 / width) + EPSILON)
            rows[pl.ds(pl.multiple_of(i * chunk, chunk), chunk), :] = (x * scale * gain[...]).astype(BF16)
            return carry

        lax.fori_loop(0, 2 * block // chunk, norm, 0)
        first = flags[1] == 0
        place[:block, :] = places(jnp.where(first, own[...], other[...]), experts).astype(BF16)
        place[block:, :] = places(jnp.where(first, other[...], own[...]), experts).astype(BF16)
        slots = select.shape[0]
        slot = iota((slots, 1), 0)
        expert = quotient(slot, 2 * capacity)
        within = slot - expert * (2 * capacity)
        second = jnp.where(within >= capacity, 1, 0)
        wanted = (within - second * capacity).astype(F32)
        there = dot_rows(ones_where(expert == iota((slots, experts), 1)), place[...])
        row_block = jnp.where(iota((slots, 2 * block), 1) >= block, 1, 0)
        select[...] = ones_where((there == wanted) & (row_block == second))

    here = out.shape[1]
    at = pl.multiple_of(step * here, here)
    out[...] = dot(select[...], rows[:, pl.ds(at, here)]).astype(BF16)


def outbox_of(flags, tokens, gain, own, other, experts, capacity):
    width = tokens.shape[1]
    block = own.shape[0]
    slots = experts * 2 * capacity
    here = 512
    return pl.pallas_call(
        partial(outbox_body, capacity=capacity, chunk=32),
        grid_spec=pltpu.PrefetchScalarGridSpec(
            num_scalar_prefetch=1,
            grid=(width // here,),
            in_specs=[
                pl.BlockSpec((2, 1, block, width), lambda i, f: (0, f[0], 0, 0)),
                pl.BlockSpec((1, width), lambda i, f: (0, 0)),
                pl.BlockSpec(own.shape, lambda i, f: (0, 0)),
                pl.BlockSpec(other.shape, lambda i, f: (0, 0)),
            ],
            out_specs=pl.BlockSpec((slots, here), lambda i, f: (0, i)),
            scratch_shapes=[
                pltpu.VMEM((2 * block, width), BF16),
                pltpu.VMEM((2 * block, experts), BF16),
                pltpu.VMEM((slots, 2 * block), BF16),
            ],
        ),
        out_shape=jax.ShapeDtypeStruct((slots, width), BF16),
        cost_estimate=pl.CostEstimate(flops=2 * slots * 2 * block * width, bytes_accessed=2 * width * (slots + 2 * block), transcendentals=0),
        name="outbox",
    )(flags, tokens.reshape(2, 2, block, width), gain.reshape(1, width), own, other)


def hidden_body(flags, arrived, gate, up, first, second, kept, sent, sums, hidden, *, capacity, chunk):
    step = pl.program_id(0)
    a = arrived[...]
    weights = (gate, up, first, second)

    @pl.when(step == 0)
    def _():
        for i, w in enumerate(weights):
            sums[i] = dot(a, w[...])

    @pl.when(step != 0)
    def _():
        for i, w in enumerate(weights):
            sums[i] += dot(a, w[...])

    @pl.when(step == pl.num_programs(0) - 1)
    def _():
        units = gate.shape[1]
        half = units // 2

        def activate(i, carry):
            at = pl.ds(pl.multiple_of(i * chunk, chunk), chunk)
            hidden[at, :units] = gated_product(sums[0, at, :], sums[1, at, :])
            hidden[at, units : units + half] = gated_product(sums[2, at, :half], sums[2, at, half:])
            hidden[at, units + half :] = gated_product(sums[3, at, :half], sums[3, at, half:])
            return carry

        lax.fori_loop(0, a.shape[0] // chunk, activate, 0)
        shape = (kept.shape[0], a.shape[0])
        row = iota((shape[0], 1), 0)
        source = row + capacity * quotient(row, capacity)
        lane = iota(shape, 1)
        kept[...] = dot(ones_where(lane == source + capacity * flags[1]), hidden[...]).astype(BF16)
        sent[...] = dot(ones_where(lane == source + capacity * (1 - flags[1])), hidden[...]).astype(BF16)


def hidden_of(flags, arrived, gate, up, first, second, capacity):
    rows, width = arrived.shape
    units = gate.shape[1]
    step = 512
    out = jax.ShapeDtypeStruct((rows // 2, 2 * units), BF16)
    weight = pl.BlockSpec((step, units), lambda k, f: (k, 0))
    whole = pl.BlockSpec(out.shape, lambda k, f: (0, 0))
    return pl.pallas_call(
        partial(hidden_body, capacity=capacity, chunk=64),
        grid_spec=pltpu.PrefetchScalarGridSpec(
            num_scalar_prefetch=1,
            grid=(width // step,),
            in_specs=[pl.BlockSpec((rows, step), lambda k, f: (0, k))] + [weight] * 4,
            out_specs=[whole, whole],
            scratch_shapes=[pltpu.VMEM((4, rows, units), F32), pltpu.VMEM((rows, 2 * units), BF16)],
        ),
        out_shape=[out, out],
        cost_estimate=pl.CostEstimate(flops=8 * rows * width * units, bytes_accessed=2 * width * (rows + 4 * units), transcendentals=0),
        name="hidden",
    )(flags, arrived, gate, up, first, second)


def down_body(kept, got, *refs, capacity):
    weights, (out, whole, wide) = refs[:10], refs[10:]
    units = whole.shape[1] // 4
    half = units // 2

    @pl.when(pl.program_id(0) == 0)
    def _():
        whole[:, :units] = kept[:, :units]
        whole[:, units : units + half] = kept[:, units : units + half]
        whole[:, units + half : 2 * units] = got[:, units + half :]
        whole[:, 2 * units : 3 * units] = got[:, :units]
        whole[:, 3 * units : 3 * units + half] = got[:, units : units + half]
        whole[:, 3 * units + half :] = kept[:, units + half :]

    for side in range(2):
        own, from_1, first_of_2, second_of_2, from_3 = (w[...] for w in weights[side::2])
        from_2 = jnp.concatenate([first_of_2, second_of_2], axis=0)
        rows = dot(whole[:, :units], own) + dot(whole[:, units : 2 * units], from_1)
        rows += dot(whole[:, 2 * units : 3 * units], from_2) + dot(whole[:, 3 * units :], from_3)
        for expert in range(rows.shape[0] // capacity):
            at = (2 * expert + side) * capacity
            wide[at : at + capacity, :] = rows[expert * capacity : (expert + 1) * capacity, :]
    out[...] = wide[...].astype(BF16)


def down_of(kept, got, shards, capacity):
    rows, units = kept.shape[0], sum(w.shape[0] for w in shards)
    width = shards[0].shape[1] // 2
    step = 256
    count = width // step
    whole = pl.BlockSpec(kept.shape, lambda n: (0, 0))
    specs, operands = [], []
    for shard in shards:
        for side in range(2):
            specs.append(pl.BlockSpec((shard.shape[0], step), lambda n, side=side: (0, n + side * count)))
            operands.append(shard)
    return pl.pallas_call(
        partial(down_body, capacity=capacity),
        grid=(count,),
        in_specs=[whole, whole] + specs,
        out_specs=pl.BlockSpec((2 * rows, step), lambda n: (0, n)),
        scratch_shapes=[pltpu.VMEM((rows, units), BF16), pltpu.VMEM((2 * rows, step), F32)],
        out_shape=jax.ShapeDtypeStruct((2 * rows, width), BF16),
        cost_estimate=pl.CostEstimate(flops=4 * rows * units * width, bytes_accessed=4 * width * (rows + units), transcendentals=0),
        name="down",
    )(kept, got, *operands)


def halves_body(flags, hidden, down, send_1, keep_1, send_3, keep_3):
    me = flags[0] + 2 * flags[1]
    block, width = send_1.shape[0] // 2, send_1.shape[1]
    targets = (
        ((keep_1, 0), (keep_3, 0)),
        ((send_1, 0), (keep_3, 1)),
        ((send_1, 1), (send_3, 1)),
        ((keep_1, 1), (send_3, 0)),
    )
    for away, sides in enumerate(targets):
        at = pl.multiple_of((me ^ away) * block, block)
        for side, (out, place) in enumerate(sides):
            product = dot(hidden[pl.ds(at, block), :], down[:, side * width : (side + 1) * width])
            out[place * block : (place + 1) * block, :] = product.astype(BF16)


def halves_of(flags, hidden, down):
    rows, width = hidden.shape[0], down.shape[1]
    out = jax.ShapeDtypeStruct((rows // 2, width // 2), BF16)
    whole = pl.BlockSpec(out.shape, lambda i, f: (0, 0))
    return pl.pallas_call(
        halves_body,
        grid_spec=pltpu.PrefetchScalarGridSpec(
            num_scalar_prefetch=1,
            grid=(1,),
            in_specs=[pl.BlockSpec(hidden.shape, lambda i, f: (0, 0)), pl.BlockSpec(down.shape, lambda i, f: (0, 0))],
            out_specs=[whole] * 4,
        ),
        out_shape=[out] * 4,
        cost_estimate=pl.CostEstimate(flops=2 * rows * width * down.shape[0], bytes_accessed=2 * width * (rows + down.shape[0]), transcendentals=0),
    )(flags, hidden, down)


def portions_body(routes, weights, mix, *, capacity, experts):
    block, slots = routes.shape[0], mix.shape[2]
    chosen = routes[...]
    expert = iota((block, experts), 1)
    weight = jnp.where(chosen[:, 0:1] == expert, weights[:, 0:1], 0.0) + jnp.where(
        chosen[:, 1:2] == expert, weights[:, 1:2], 0.0
    )
    upper = weight.astype(BF16)
    lower = (weight - upper.astype(F32)).astype(BF16)
    lane = iota((experts, slots), 1)
    unfold = ones_where(quotient(lane, 2 * capacity) == iota((experts, slots), 0))
    lane = iota((1, slots), 1)
    within = lane - quotient(lane, 2 * capacity) * (2 * capacity)
    second = jnp.where(within >= capacity, 1, 0)
    wanted = (within - second * capacity).astype(F32)
    hit = dot(places(chosen, experts).astype(BF16), unfold) == wanted
    for part, values in enumerate((upper, lower)):
        there = dot(values, unfold)
        for side in range(2):
            mix[side, part * block : (part + 1) * block, :] = jnp.where(
                hit & (second == side), there, 0.0
            ).astype(BF16)


def portions_of(routes, weights, experts, capacity):
    block, slots = routes.shape[0], 2 * experts * capacity
    return pl.pallas_call(
        partial(portions_body, capacity=capacity, experts=experts),
        out_shape=jax.ShapeDtypeStruct((2, 2 * block, slots), BF16),
        cost_estimate=pl.CostEstimate(flops=6 * block * slots * experts, bytes_accessed=8 * block * slots, transcendentals=0),
        name="portions",
    )(routes, weights)


def mix_body(portions, returned, *refs):
    shared, out = refs[:-1], refs[-1]
    block, step = out.shape[0], returned.shape[1]
    at = pl.program_id(0) * step
    both = dot(portions[...], returned[...])
    for side in range(2):
        total = both[2 * side * block : (2 * side + 1) * block] + both[(2 * side + 1) * block : (2 * side + 2) * block]
        for part in shared[3 * side : 3 * side + 3]:
            total += part[...].astype(F32)
        here = pl.multiple_of(at + side * (out.shape[1] // 2), step)
        out[:, pl.ds(here, step)] = total.astype(BF16)


def mixed_of(portions, returned, shared):
    slots, width = returned.shape
    block = portions.shape[1] // 2
    step = 512
    count = width // step
    portions = portions.reshape(4 * block, slots)
    return pl.pallas_call(
        mix_body,
        grid=(count,),
        in_specs=[
            pl.BlockSpec(portions.shape, lambda n: (0, 0)),
            pl.BlockSpec((slots, step), lambda n: (0, n)),
        ]
        + [pl.BlockSpec((block, step), lambda n: (0, n))] * 6,
        out_specs=pl.BlockSpec((block, 2 * width), lambda n: (0, 0)),
        out_shape=jax.ShapeDtypeStruct((block, 2 * width), BF16),
        cost_estimate=pl.CostEstimate(flops=8 * block * slots * width, bytes_accessed=2 * width * (slots + 8 * block), transcendentals=0),
        name="mix",
    )(portions, returned, *shared)


def sum_body(*refs):
    parts, out = refs[:-1], refs[-1]
    width = out.shape[1] // 2
    for side in range(2):
        total = sum(part[...].astype(F32) for part in parts[3 * side : 3 * side + 3])
        out[:, side * width : (side + 1) * width] = total.astype(BF16)


def sum_of(parts):
    block, width = parts[2].shape
    rows = 32
    return pl.pallas_call(
        sum_body,
        grid=(block // rows,),
        in_specs=[pl.BlockSpec((rows, width), lambda i: (i, 0))] * 6,
        out_specs=pl.BlockSpec((rows, 2 * width), lambda i: (i, 0)),
        out_shape=jax.ShapeDtypeStruct((block, 2 * width), BF16),
        cost_estimate=pl.CostEstimate(flops=4 * block * width, bytes_accessed=16 * block * width, transcendentals=0),
        name="sum",
    )(*parts)


def gated_of(value_in, gate_in):
    return (value_in.astype(F32) * jax.nn.sigmoid(gate_in.astype(F32))).astype(BF16)


def convolved(before, gated, conv_taps, conv_bias):
    length = gated.shape[0]
    padded = jnp.concatenate([before, gated], axis=0).astype(F32)
    filtered = jnp.zeros(gated.shape, F32) + conv_bias[None, :]
    for tap_index in range(conv_taps.shape[0]):
        filtered = filtered + conv_taps[tap_index][None, :] * padded[tap_index : tap_index + length]
    return filtered


def two_swaps(send_1, keep_1, send_3, keep_3):
    block = send_1.shape[0] // 2
    left_1 = swapped(send_1, "tp", 1)
    right_1 = swapped(send_3, "tp", 3)
    left_on = (keep_1[block:].astype(F32) + left_1[block:].astype(F32)).astype(BF16)
    right_on = (keep_3[block:].astype(F32) + right_1[block:].astype(F32)).astype(BF16)
    left_2 = swapped(left_on, "tp", 3)
    right_2 = swapped(right_on, "tp", 1)
    return keep_1, left_1, left_2, keep_3, right_1, right_2


def per_device(
    value_in,
    gate_in,
    conv_taps,
    conv_bias,
    ln_gain,
    ln_bias,
    out_proj,
    tokens_b,
    norm_gain,
    routes,
    route_weights,
    expert_gate,
    expert_up,
    expert_down,
    shared_gate,
    shared_up,
    shared_down,
):
    tp_count = lax.axis_size("tp")
    ep_count = lax.axis_size("ep")
    me = lax.axis_index("tp")
    flags = jnp.stack([me & 1, me >> 1]).astype(jnp.int32)
    rows_own, top_count = routes.shape
    capacity = max(2, 3 * rows_own * top_count // (2 * ep_count))
    width = tokens_b.shape[1]
    gate_local, up_local, down_local = expert_gate[0], expert_up[0], expert_down[0]
    half = gate_local.shape[1] // 2
    down_half = down_local.shape[0] // 2

    other_routes = swapped(routes, "tp", 2)

    rim = value_in.shape[0] - (conv_taps.shape[0] - 1)
    tail = gated_of(value_in[rim:], gate_in[rim:])
    before = shifted(tail, "ep", 1)

    down_1 = swapped(down_local, "tp", 1)
    down_3 = swapped(down_local, "tp", 3)

    outbox = outbox_of(flags, tokens_b, norm_gain, routes, other_routes, ep_count, capacity)
    arrived = lax.all_to_all(
        outbox.reshape(ep_count, 2 * capacity, width), "ep", split_axis=0, concat_axis=0, tiled=True
    ).reshape(2 * capacity * ep_count, width)
    tokens_b, value_in, gate_in, gate_sent, up_sent, outbox = lax.optimization_barrier(
        (tokens_b, value_in, gate_in, gate_local, up_local, outbox)
    )

    first = jnp.concatenate([gate_sent[:, :half], up_sent[:, :half]], axis=1)
    second = jnp.concatenate([gate_sent[:, half:], up_sent[:, half:]], axis=1)
    first_of_1 = swapped(first, "tp", 1)
    second_of_3 = swapped(second, "tp", 3)
    down_2a = swapped(down_3[:down_half], "tp", 1)
    down_2b = swapped(down_1[down_half:], "tp", 3)

    filtered = convolved(before, gated_of(value_in, gate_in), conv_taps, conv_bias)
    sums = jnp.stack([jnp.sum(filtered, axis=1), jnp.sum(filtered * filtered, axis=1)])
    other_sums = [swapped(sums, "tp", bits) for bits in (1, 2, 3)]

    features = tokens_b.astype(F32)
    normed_b = (
        features
        * lax.rsqrt(jnp.mean(features * features, axis=1, keepdims=True) + EPSILON)
        * norm_gain
    ).astype(BF16)
    hidden_shared = gated_product(dot(normed_b, shared_gate), dot(normed_b, shared_up))
    send_1, keep_1, send_3, keep_3 = halves_of(flags, hidden_shared, shared_down)

    *other_sums, hidden_shared, send_1, send_3 = lax.optimization_barrier(
        (*other_sums, hidden_shared, send_1, send_3)
    )
    total = sums + other_sums[0] + (other_sums[1] + other_sums[2])
    channel_count = filtered.shape[1] * tp_count
    average = total[0] / channel_count
    variance = total[1] / channel_count - average * average
    normed_a = (filtered - average[:, None]) * lax.rsqrt(
        variance[:, None] + EPSILON
    ) * ln_gain + ln_bias
    activated = jax.nn.silu(normed_a).astype(BF16)
    mixer_parts = halves_of(flags, activated, out_proj)

    kept, sent = hidden_of(flags, arrived, gate_local, up_local, first_of_1, second_of_3, capacity)
    got = swapped(sent, "tp", 2)

    shared_sums = two_swaps(send_1, keep_1, send_3, keep_3)
    mixer_sums = two_swaps(*mixer_parts)

    expert_rows = down_of(kept, got, (down_local, down_1, down_2a, down_2b, down_3), capacity)
    returned = lax.all_to_all(
        expert_rows.reshape(ep_count, 2 * capacity, width // 2), "ep", split_axis=0, concat_axis=0, tiled=True
    ).reshape(2 * capacity * ep_count, width // 2)
    portions = portions_of(routes, route_weights, ep_count, capacity)
    experts_out = mixed_of(portions, returned, shared_sums)
    *mixer_sums, experts_out = lax.optimization_barrier((*mixer_sums, experts_out))
    mixer_rows = sum_of(mixer_sums)
    return (mixer_rows, experts_out)


def solution(mesh):
    return jax.shard_map(
        per_device,
        mesh=mesh,
        in_specs=(
            P("ep", "tp"),
            P("ep", "tp"),
            P(None, "tp"),
            P("tp"),
            P("tp"),
            P("tp"),
            P("tp", None),
            P("ep", None),
            P(),
            P(("ep", "tp"), None),
            P(("ep", "tp"), None),
            P("ep", None, "tp"),
            P("ep", None, "tp"),
            P("ep", "tp", None),
            P(None, "tp"),
            P(None, "tp"),
            P("tp", None),
        ),
        out_specs=(P(("ep", "tp"), None), P(("ep", "tp"), None)),
        check_vma=False,
    )
```

```python
from functools import partial

import jax
import jax.numpy as jnp
from jax import lax
from jax.experimental import pallas as pl
from jax.experimental.pallas import tpu as pltpu
from jax.sharding import PartitionSpec as P


EPSILON = 1e-06
BF16, F32 = jnp.bfloat16, jnp.float32


def shifted(x, axis, by):
    devices = lax.axis_size(axis)
    pairs = [(i, i + by) for i in range(devices) if 0 <= i + by < devices]
    return lax.ppermute(x, axis, pairs)


def swapped(x, axis, bits):
    return lax.ppermute(x, axis, [(i, i ^ bits) for i in range(lax.axis_size(axis))])


def dot(a, b):
    return jnp.dot(a, b, preferred_element_type=F32)


def gated_product(gate, up):
    return (jax.nn.silu(gate) * up).astype(BF16)


def iota(shape, dim):
    return lax.broadcasted_iota(jnp.int32, shape, dim)


def ones_where(mask):
    return jnp.where(mask, 1.0, 0.0).astype(BF16)


def quotient(x, by):
    return (x * (65536 // by + 1)) >> 16


def dot_columns(a, b):
    return lax.dot_general(a, b, (((0,), (0,)), ((), ())), preferred_element_type=F32)


def places(routes, experts):
    rows = routes.shape[1]
    expert = iota((experts, rows), 0)
    named = (routes[0:1, :] == expert) | (routes[1:2, :] == expert)
    earlier = ones_where(iota((rows, rows), 0) < iota((rows, rows), 1))
    return jnp.where(named, dot(ones_where(named), earlier), -1.0)


def outbox_body(flags, tokens, gain, own, other, out, rows, place, select, *, capacity, chunk):
    step = pl.program_id(0)
    block, width = own.shape[1], gain.shape[1]
    experts = place.shape[0]

    @pl.when(step == 0)
    def _():
        def norm(i, carry):
            at = pl.multiple_of((i % (block // chunk)) * chunk, chunk)
            x = tokens[i // (block // chunk), 0, pl.ds(at, chunk), :].astype(F32)
            scale = lax.rsqrt(jnp.sum(x * x, axis=1, keepdims=True) * (1.0 / width) + EPSILON)
            rows[pl.ds(pl.multiple_of(i * chunk, chunk), chunk), :] = (x * scale * gain[...]).astype(BF16)
            return carry

        lax.fori_loop(0, 2 * block // chunk, norm, 0, unroll=2)
        first = flags[1] == 0
        place[:, :block] = places(jnp.where(first, own[...], other[...]), experts).astype(BF16)
        place[:, block:] = places(jnp.where(first, other[...], own[...]), experts).astype(BF16)
        slots = select.shape[0]
        slot = iota((slots, 1), 0)
        expert = quotient(slot, 2 * capacity)
        within = slot - expert * (2 * capacity)
        second = jnp.where(within >= capacity, 1, 0)
        wanted = (within - second * capacity).astype(F32)
        there = dot(ones_where(expert == iota((slots, experts), 1)), place[...])
        row_block = jnp.where(iota((slots, 2 * block), 1) >= block, 1, 0)
        select[...] = ones_where((there == wanted) & (row_block == second))

    here = out.shape[1]
    at = pl.multiple_of(step * here, here)
    out[...] = dot(select[...], rows[:, pl.ds(at, here)]).astype(BF16)


def outbox_of(flags, tokens, gain, own, other, experts, capacity):
    width = tokens.shape[1]
    block = own.shape[1]
    slots = experts * 2 * capacity
    here = 512
    return pl.pallas_call(
        partial(outbox_body, capacity=capacity, chunk=32),
        grid_spec=pltpu.PrefetchScalarGridSpec(
            num_scalar_prefetch=1,
            grid=(width // here,),
            in_specs=[
                pl.BlockSpec((2, 1, block, width), lambda i, f: (0, f[0], 0, 0)),
                pl.BlockSpec((1, width), lambda i, f: (0, 0)),
                pl.BlockSpec(own.shape, lambda i, f: (0, 0)),
                pl.BlockSpec(other.shape, lambda i, f: (0, 0)),
            ],
            out_specs=pl.BlockSpec((slots, here), lambda i, f: (0, i)),
            scratch_shapes=[
                pltpu.VMEM((2 * block, width), BF16),
                pltpu.VMEM((experts, 2 * block), BF16),
                pltpu.VMEM((slots, 2 * block), BF16),
            ],
        ),
        out_shape=jax.ShapeDtypeStruct((slots, width), BF16),
        cost_estimate=pl.CostEstimate(flops=2 * slots * 2 * block * width, bytes_accessed=2 * width * (slots + 2 * block), transcendentals=0),
        name="outbox",
    )(flags, tokens.reshape(2, 2, block, width), gain.reshape(1, width), own, other)


def hidden_body(flags, arrived, gate, up, first, second, kept, sent, sums, hidden, *, capacity, chunk):
    step = pl.program_id(0)
    a = arrived[...]
    weights = (gate, up, first, second)

    @pl.when(step == 0)
    def _():
        for i, w in enumerate(weights):
            sums[i] = dot(a, w[...])

    @pl.when(step != 0)
    def _():
        for i, w in enumerate(weights):
            sums[i] += dot(a, w[...])

    @pl.when(step == pl.num_programs(0) - 1)
    def _():
        units = gate.shape[1]
        half = units // 2

        def activate(i, carry):
            at = pl.ds(pl.multiple_of(i * chunk, chunk), chunk)
            hidden[at, :units] = gated_product(sums[0, at, :], sums[1, at, :])
            hidden[at, units : units + half] = gated_product(sums[2, at, :half], sums[2, at, half:])
            hidden[at, units + half :] = gated_product(sums[3, at, :half], sums[3, at, half:])
            return carry

        lax.fori_loop(0, a.shape[0] // chunk, activate, 0)
        shape = (kept.shape[0], a.shape[0])
        row = iota((shape[0], 1), 0)
        source = row + capacity * quotient(row, capacity)
        lane = iota(shape, 1)
        kept[...] = dot(ones_where(lane == source + capacity * flags[1]), hidden[...]).astype(BF16)
        sent[...] = dot(ones_where(lane == source + capacity * (1 - flags[1])), hidden[...]).astype(BF16)


def hidden_of(flags, arrived, gate, up, first, second, capacity):
    rows, width = arrived.shape
    units = gate.shape[1]
    step = 512
    out = jax.ShapeDtypeStruct((rows // 2, 2 * units), BF16)
    weight = pl.BlockSpec((step, units), lambda k, f: (k, 0))
    whole = pl.BlockSpec(out.shape, lambda k, f: (0, 0))
    return pl.pallas_call(
        partial(hidden_body, capacity=capacity, chunk=64),
        grid_spec=pltpu.PrefetchScalarGridSpec(
            num_scalar_prefetch=1,
            grid=(width // step,),
            in_specs=[pl.BlockSpec((rows, step), lambda k, f: (0, k))] + [weight] * 4,
            out_specs=[whole, whole],
            scratch_shapes=[pltpu.VMEM((4, rows, units), F32), pltpu.VMEM((rows, 2 * units), BF16)],
        ),
        out_shape=[out, out],
        cost_estimate=pl.CostEstimate(flops=8 * rows * width * units, bytes_accessed=2 * width * (rows + 4 * units), transcendentals=0),
        name="hidden",
    )(flags, arrived, gate, up, first, second)


def down_body(kept, got, *refs, capacity):
    weights, (out, whole, wide) = refs[:10], refs[10:]
    units = whole.shape[1] // 4
    half = units // 2

    @pl.when(pl.program_id(0) == 0)
    def _():
        whole[:, :units] = kept[:, :units]
        whole[:, units : units + half] = kept[:, units : units + half]
        whole[:, units + half : 2 * units] = got[:, units + half :]
        whole[:, 2 * units : 3 * units] = got[:, :units]
        whole[:, 3 * units : 3 * units + half] = got[:, units : units + half]
        whole[:, 3 * units + half :] = kept[:, units + half :]

    for side in range(2):
        own, from_1, first_of_2, second_of_2, from_3 = (w[...] for w in weights[side::2])
        from_2 = jnp.concatenate([first_of_2, second_of_2], axis=0)
        rows = dot(whole[:, :units], own) + dot(whole[:, units : 2 * units], from_1)
        rows += dot(whole[:, 2 * units : 3 * units], from_2) + dot(whole[:, 3 * units :], from_3)
        for expert in range(rows.shape[0] // capacity):
            at = (2 * expert + side) * capacity
            wide[at : at + capacity, :] = rows[expert * capacity : (expert + 1) * capacity, :]
    out[...] = wide[...].astype(BF16)


def down_of(kept, got, shards, capacity):
    rows, units = kept.shape[0], sum(w.shape[0] for w in shards)
    width = shards[0].shape[1] // 2
    step = 256
    count = width // step
    whole = pl.BlockSpec(kept.shape, lambda n: (0, 0))
    specs, operands = [], []
    for shard in shards:
        for side in range(2):
            specs.append(pl.BlockSpec((shard.shape[0], step), lambda n, side=side: (0, n + side * count)))
            operands.append(shard)
    return pl.pallas_call(
        partial(down_body, capacity=capacity),
        grid=(count,),
        in_specs=[whole, whole] + specs,
        out_specs=pl.BlockSpec((2 * rows, step), lambda n: (0, n)),
        scratch_shapes=[pltpu.VMEM((rows, units), BF16), pltpu.VMEM((2 * rows, step), F32)],
        out_shape=jax.ShapeDtypeStruct((2 * rows, width), BF16),
        cost_estimate=pl.CostEstimate(flops=4 * rows * units * width, bytes_accessed=4 * width * (rows + units), transcendentals=0),
        name="down",
    )(kept, got, *operands)


def halves_body(flags, hidden, down, send_1, keep_1, send_3, keep_3):
    me = flags[0] + 2 * flags[1]
    block, width = send_1.shape[0] // 2, send_1.shape[1]
    targets = (
        ((keep_1, 0), (keep_3, 0)),
        ((send_1, 0), (keep_3, 1)),
        ((send_1, 1), (send_3, 1)),
        ((keep_1, 1), (send_3, 0)),
    )
    for away, sides in enumerate(targets):
        at = pl.multiple_of((me ^ away) * block, block)
        for side, (out, place) in enumerate(sides):
            product = dot(hidden[pl.ds(at, block), :], down[:, side * width : (side + 1) * width])
            out[place * block : (place + 1) * block, :] = product.astype(BF16)


def halves_of(flags, hidden, down):
    rows, width = hidden.shape[0], down.shape[1]
    out = jax.ShapeDtypeStruct((rows // 2, width // 2), BF16)
    whole = pl.BlockSpec(out.shape, lambda i, f: (0, 0))
    return pl.pallas_call(
        halves_body,
        grid_spec=pltpu.PrefetchScalarGridSpec(
            num_scalar_prefetch=1,
            grid=(1,),
            in_specs=[pl.BlockSpec(hidden.shape, lambda i, f: (0, 0)), pl.BlockSpec(down.shape, lambda i, f: (0, 0))],
            out_specs=[whole] * 4,
        ),
        out_shape=[out] * 4,
        cost_estimate=pl.CostEstimate(flops=2 * rows * width * down.shape[0], bytes_accessed=2 * width * (rows + down.shape[0]), transcendentals=0),
    )(flags, hidden, down)


def portions_body(routes, weights, mix, *, capacity, experts):
    block, slots = routes.shape[1], mix.shape[1]
    chosen = routes[...]
    expert = iota((experts, block), 0)
    weight = jnp.where(chosen[0:1, :] == expert, weights[0:1, :], 0.0) + jnp.where(
        chosen[1:2, :] == expert, weights[1:2, :], 0.0
    )
    upper = weight.astype(BF16)
    lower = (weight - upper.astype(F32)).astype(BF16)
    lane = iota((experts, slots), 1)
    unfold = ones_where(quotient(lane, 2 * capacity) == iota((experts, slots), 0))
    lane = iota((1, slots), 1)
    within = lane - quotient(lane, 2 * capacity) * (2 * capacity)
    second = jnp.where(within >= capacity, 1, 0)
    wanted = (within - second * capacity).astype(F32)
    hit = dot_columns(places(chosen, experts).astype(BF16), unfold) == wanted
    for part, values in enumerate((upper, lower)):
        there = dot_columns(values, unfold)
        for side in range(2):
            at = (2 * side + part) * block
            mix[at : at + block, :] = jnp.where(hit & (second == side), there, 0.0).astype(BF16)


def portions_of(routes, weights, experts, capacity):
    block, slots = routes.shape[1], 2 * experts * capacity
    return pl.pallas_call(
        partial(portions_body, capacity=capacity, experts=experts),
        out_shape=jax.ShapeDtypeStruct((4 * block, slots), BF16),
        cost_estimate=pl.CostEstimate(flops=6 * block * slots * experts, bytes_accessed=8 * block * slots, transcendentals=0),
        name="portions",
    )(routes, weights)


def mix_body(portions, returned, *refs):
    shared, out = refs[:-1], refs[-1]
    block, step = out.shape[0], returned.shape[1]
    at = pl.program_id(0) * step
    both = dot(portions[...], returned[...])
    for side in range(2):
        total = both[2 * side * block : (2 * side + 1) * block] + both[(2 * side + 1) * block : (2 * side + 2) * block]
        for part in shared[3 * side : 3 * side + 3]:
            total += part[...].astype(F32)
        here = pl.multiple_of(at + side * (out.shape[1] // 2), step)
        out[:, pl.ds(here, step)] = total.astype(BF16)


def mixed_of(portions, returned, shared):
    slots, width = returned.shape
    block = portions.shape[0] // 4
    step = 512
    count = width // step
    return pl.pallas_call(
        mix_body,
        grid=(count,),
        in_specs=[
            pl.BlockSpec(portions.shape, lambda n: (0, 0)),
            pl.BlockSpec((slots, step), lambda n: (0, n)),
        ]
        + [pl.BlockSpec((block, step), lambda n: (0, n))] * 6,
        out_specs=pl.BlockSpec((block, 2 * width), lambda n: (0, 0)),
        out_shape=jax.ShapeDtypeStruct((block, 2 * width), BF16),
        cost_estimate=pl.CostEstimate(flops=8 * block * slots * width, bytes_accessed=2 * width * (slots + 8 * block), transcendentals=0),
        name="mix",
    )(portions, returned, *shared)


def gated_of(value_in, gate_in):
    return (value_in.astype(F32) * jax.nn.sigmoid(gate_in.astype(F32))).astype(BF16)


def convolved(before, gated, conv_taps, conv_bias):
    length = gated.shape[0]
    padded = jnp.concatenate([before, gated], axis=0).astype(F32)
    filtered = jnp.zeros(gated.shape, F32) + conv_bias[None, :]
    for tap_index in range(conv_taps.shape[0]):
        filtered = filtered + conv_taps[tap_index][None, :] * padded[tap_index : tap_index + length]
    return filtered


def two_swaps(send_1, keep_1, send_3, keep_3):
    block = send_1.shape[0] // 2
    left_1 = swapped(send_1, "tp", 1)
    right_1 = swapped(send_3, "tp", 3)
    left_on = (keep_1[block:].astype(F32) + left_1[block:].astype(F32)).astype(BF16)
    right_on = (keep_3[block:].astype(F32) + right_1[block:].astype(F32)).astype(BF16)
    left_2 = swapped(left_on, "tp", 3)
    right_2 = swapped(right_on, "tp", 1)
    return keep_1, left_1, left_2, keep_3, right_1, right_2


def per_device(
    value_in,
    gate_in,
    conv_taps,
    conv_bias,
    ln_gain,
    ln_bias,
    out_proj,
    tokens_b,
    norm_gain,
    routes,
    route_weights,
    expert_gate,
    expert_up,
    expert_down,
    shared_gate,
    shared_up,
    shared_down,
):
    tp_count = lax.axis_size("tp")
    ep_count = lax.axis_size("ep")
    me = lax.axis_index("tp")
    flags = jnp.stack([me & 1, me >> 1]).astype(jnp.int32)
    rows_own, top_count = routes.shape
    capacity = max(2, 3 * rows_own * top_count // (2 * ep_count))
    width = tokens_b.shape[1]
    gate_local, up_local, down_local = expert_gate[0], expert_up[0], expert_down[0]
    half = gate_local.shape[1] // 2
    down_half = down_local.shape[0] // 2

    routes = routes.T
    other_routes = swapped(routes, "tp", 2)

    rim = value_in.shape[0] - (conv_taps.shape[0] - 1)
    tail = gated_of(value_in[rim:], gate_in[rim:])
    before = shifted(tail, "ep", 1)

    down_1 = swapped(down_local, "tp", 1)
    down_3 = swapped(down_local, "tp", 3)

    outbox = outbox_of(flags, tokens_b, norm_gain, routes, other_routes, ep_count, capacity)
    arrived = lax.all_to_all(
        outbox.reshape(ep_count, 2 * capacity, width), "ep", split_axis=0, concat_axis=0, tiled=True
    ).reshape(2 * capacity * ep_count, width)
    tokens_b, value_in, gate_in, gate_sent, up_sent, outbox = lax.optimization_barrier(
        (tokens_b, value_in, gate_in, gate_local, up_local, outbox)
    )

    first = jnp.concatenate([gate_sent[:, :half], up_sent[:, :half]], axis=1)
    second = jnp.concatenate([gate_sent[:, half:], up_sent[:, half:]], axis=1)
    first_of_1 = swapped(first, "tp", 1)
    second_of_3 = swapped(second, "tp", 3)
    down_2a = swapped(down_3[:down_half], "tp", 1)
    down_2b = swapped(down_1[down_half:], "tp", 3)

    filtered = convolved(before, gated_of(value_in, gate_in), conv_taps, conv_bias)
    sums = jnp.stack([jnp.sum(filtered, axis=1), jnp.sum(filtered * filtered, axis=1)])
    other_sums = [swapped(sums, "tp", bits) for bits in (1, 2, 3)]

    features = tokens_b.astype(F32)
    normed_b = (
        features
        * lax.rsqrt(jnp.mean(features * features, axis=1, keepdims=True) + EPSILON)
        * norm_gain
    ).astype(BF16)
    hidden_shared = gated_product(dot(normed_b, shared_gate), dot(normed_b, shared_up))
    send_1, keep_1, send_3, keep_3 = halves_of(flags, hidden_shared, shared_down)

    *other_sums, hidden_shared, send_1, send_3 = lax.optimization_barrier(
        (*other_sums, hidden_shared, send_1, send_3)
    )
    total = sums + other_sums[0] + (other_sums[1] + other_sums[2])
    channel_count = filtered.shape[1] * tp_count
    average = total[0] / channel_count
    variance = total[1] / channel_count - average * average
    normed_a = (filtered - average[:, None]) * lax.rsqrt(
        variance[:, None] + EPSILON
    ) * ln_gain + ln_bias
    activated = jax.nn.silu(normed_a).astype(BF16)
    mixer_parts = halves_of(flags, activated, out_proj)

    kept, sent = hidden_of(flags, arrived, gate_local, up_local, first_of_1, second_of_3, capacity)
    got = swapped(sent, "tp", 2)

    shared_sums = two_swaps(send_1, keep_1, send_3, keep_3)
    mixer_sums = two_swaps(*mixer_parts)

    expert_rows = down_of(kept, got, (down_local, down_1, down_2a, down_2b, down_3), capacity)
    returned = lax.all_to_all(
        expert_rows.reshape(ep_count, 2 * capacity, width // 2), "ep", split_axis=0, concat_axis=0, tiled=True
    ).reshape(2 * capacity * ep_count, width // 2)
    portions = portions_of(routes, route_weights.T, ep_count, capacity)
    experts_out = mixed_of(portions, returned, shared_sums)
    own = [mixer_sums[i][:rows_own].astype(F32) + mixer_sums[i + 1][:rows_own].astype(F32) for i in (0, 3)]
    own = jnp.concatenate(own, axis=1)
    own, left_2, right_2, experts_out = lax.optimization_barrier((own, mixer_sums[2], mixer_sums[5], experts_out))
    mixer_rows = (own + jnp.concatenate([left_2, right_2], axis=1).astype(F32)).astype(BF16)
    return (mixer_rows, experts_out)


def solution(mesh):
    return jax.shard_map(
        per_device,
        mesh=mesh,
        in_specs=(
            P("ep", "tp"),
            P("ep", "tp"),
            P(None, "tp"),
            P("tp"),
            P("tp"),
            P("tp"),
            P("tp", None),
            P("ep", None),
            P(),
            P(("ep", "tp"), None),
            P(("ep", "tp"), None),
            P("ep", None, "tp"),
            P("ep", None, "tp"),
            P("ep", "tp", None),
            P(None, "tp"),
            P(None, "tp"),
            P("tp", None),
        ),
        out_specs=(P(("ep", "tp"), None), P(("ep", "tp"), None)),
        check_vma=False,
    )
```
